32 devices in a mesh: ep: 8 (over z, core), tp: 4 (over y, x).
Axes of the slice: x: 2, y: 2, z: 4, core: 2. Of those that a mesh axis runs over, the one named last changes fastest.
Arguments:
- query_in: bfloat16 [1024, 8192], P('tp', 'ep'), may hold values from -6 to 6
- key_in: bfloat16 [1024, 8192], P('tp', 'ep'), may hold values from -10 to 10
- value_in: bfloat16 [1024, 8192], P('tp', 'ep'), may hold values from -6 to 6
- erase_pre: bfloat16 [1024, 8192], P('tp', 'ep'), may hold values from -8 to 5
- decay_pre: bfloat16 [1024, 8192], P('tp', 'ep'), may hold values from -30 to 4.5
- mix_gain: float32 [1024], P('tp'), may hold values from 0.1 to 1.9
- expert_in: bfloat16 [2048, 2048], P('ep'), may hold values from -6 to 6
- expert_gain: float32 [2048], replicated, may hold values from 0.1 to 1.9
- routes: int32 [2048, 2], P('ep'), may hold values from 0 to 7, all different within a row; in each aligned block of 256 rows (0 to 255, 256 to 511, ...) at most 96 rows name the same one
- route_weight: float32 [2048, 2], P('ep'), may hold values from 0.1 to 1
- gate_weight: bfloat16 [8, 2048, 3584], P('ep', None, 'tp'), may hold values from -0.125 to 0.125
- up_weight: bfloat16 [8, 2048, 3584], P('ep', None, 'tp'), may hold values from -0.125 to 0.125
- down_weight: bfloat16 [8, 3584, 2048], P('ep', 'tp'), may hold values from -0.09375 to 0.09375
Outputs:
- mixer_out: bfloat16 [1024, 8192], P('tp', 'ep')
- expert_out: bfloat16 [2048, 2048], P('ep', 'tp')
The draws below stay inside these ranges and needn't reach their ends.
Inputs may be any that keep to these rules, and one draw needn't show every extreme that they name: `routes`: A row's 2 experts differ. Within the 256 rows of one index of ep, every expert is named at most 96 times; in some of these aligned blocks one expert is named exactly 96 times.
All inputs are finite; a program needn't handle non-finite values.
Results may differ from the reference program's by a relative error of at most 0.015.
Values may be sent and summed in bfloat16 or wider, within the bound.
A program may use at most 128 MiB of HBM per device.

```python
import math
import jax
import jax.numpy as jnp
import numpy as np
from jax import lax

D = 2048
HEADS = 16
HEAD_DIM = 64
WIDTH = 1024
FFX = 3584
TOPK = 2
BLOCK_TOKENS = 64
TOK_EP = 256
SEQ_DEV = 1024
EXPERTS = 8
CAP = 96
TOKENS = 2048
SEQUENCE_LENGTH = 8192
N_EP = 8
N_TP = 4


spike_count = 3


spike_total = 2


aligned_scale = 2.0


def head_classes(key):
    head_count = WIDTH // HEAD_DIM
    fast_count = head_count // 2
    order = jax.random.permutation(jax.random.fold_in(key, 101), head_count)
    return jnp.repeat(order < fast_count, HEAD_DIM)


def strong_cells(key):
    quick_decay_channels = head_classes(key)
    total_blocks = SEQUENCE_LENGTH // BLOCK_TOKENS
    selected_experts = jax.random.randint(jax.random.fold_in(key, 202), (spike_total,), 0, total_blocks)
    spike_token_rows = jnp.any((jnp.arange(SEQUENCE_LENGTH) // BLOCK_TOKENS)[:, None] == selected_experts[None, :], axis=1)
    return jnp.logical_or(quick_decay_channels[None, :], spike_token_rows[:, None])


def draw_key_in(key, part):
    random_keys = jax.random.split(jax.random.fold_in(key, 303), 3)
    strong = strong_cells(key)
    own_part = jnp.clip(jax.random.normal(random_keys[0], (SEQUENCE_LENGTH, WIDTH), jnp.float32), -4.0, 4.0)
    direction = jnp.clip(jax.random.normal(random_keys[1], (WIDTH,), jnp.float32), -3.0, 3.0)
    signs = (jax.random.randint(random_keys[2], (SEQUENCE_LENGTH,), 0, 2) * 2 - 1).astype(jnp.float32)
    shared = aligned_scale * signs[:, None] * direction[None, :]
    keys_drawn = jnp.where(strong, own_part + shared, own_part)
    return jnp.clip(keys_drawn, -10.0, 10.0).T.astype(jnp.bfloat16)


def draw_erase_pre(key, part):
    random_keys = jax.random.split(jax.random.fold_in(key, 404), 2)
    strong = strong_cells(key)
    high_value = jnp.clip(2.5 + 1.2 * jax.random.normal(random_keys[0], (SEQUENCE_LENGTH, WIDTH), jnp.float32), 0.5, 5.0)
    low_value = jnp.clip(-7.0 + 0.5 * jax.random.normal(random_keys[1], (SEQUENCE_LENGTH, WIDTH), jnp.float32), -8.0, -6.0)
    return jnp.where(strong, high_value, low_value).T.astype(jnp.bfloat16)


def draw_decay_pre(key, part):
    random_keys = jax.random.split(key, 7)
    slow_mask = jnp.logical_not(head_classes(key))
    slow_rate = jnp.log(1.0 / SEQUENCE_LENGTH) + jax.random.uniform(random_keys[1], (WIDTH,), jnp.float32, -1.0, 1.0)
    fast_rate = jax.random.uniform(random_keys[2], (WIDTH,), jnp.float32, jnp.log(1.0 / 100.0), jnp.log(1.0 / 30.0))
    base_rate = jnp.where(slow_mask, slow_rate, fast_rate)
    device_shift = jnp.repeat(jax.random.uniform(random_keys[3], (SEQUENCE_LENGTH // SEQ_DEV, 1), jnp.float32, -0.7, 0.7), SEQ_DEV, axis=0)
    jitter = jnp.clip(jax.random.normal(random_keys[4], (SEQUENCE_LENGTH, WIDTH), jnp.float32), -3.0, 3.0) * 0.6
    logarithm_rate = jnp.minimum(base_rate[None, :] + device_shift + jitter, -1.0)
    locations = jax.random.randint(random_keys[5], (spike_count,), 0, SEQUENCE_LENGTH)
    spike_rows = jnp.any(jnp.arange(SEQUENCE_LENGTH)[:, None] == locations[None, :], axis=1)
    dropped_share = jax.random.uniform(random_keys[6], (SEQUENCE_LENGTH, WIDTH), jnp.float32, 0.2, 0.45)
    spike_rate = jnp.log(-jnp.log(1.0 - dropped_share))
    logarithm_rate = jnp.where(spike_rows[:, None], spike_rate, logarithm_rate)
    return (-jnp.log(jnp.expm1(-logarithm_rate - 0.5))).T.astype(jnp.bfloat16)


def block_levels(key, extent, shards, low, top_value):
    level = 1.0
    for axis_at, parts in shards:
        heights = jax.random.uniform(jax.random.fold_in(jax.random.fold_in(key, 6), axis_at), (parts,), jnp.float32, low / len(shards), top_value / len(shards))
        level = level * jnp.repeat(jnp.exp(heights), extent[axis_at] // parts).reshape((-1,) + (1,) * (len(extent) - 1 - axis_at))
    return level


def shared_out(rng, own, number, rows, amount, top, most, lean):
    order = jax.random.permutation(rng, amount)
    crowded, usual = load_shares(amount, rows * top, most, lean, True), load_shares(amount, rows * top, most, lean, False)
    places = jnp.arange(amount)

    def named(sizes, rotation):
        used = int((sizes > 0).sum())
        fixed = max(1, used // 4)
        passed = fixed + (places - fixed + rotation * (used - fixed)) % max(1, amount - fixed)
        return jnp.zeros((amount,), jnp.int32).at[order[jnp.where(places < fixed, places, passed)]].set(jnp.asarray(sizes, jnp.int32))

    sizes = jnp.where(number % 4 == 0, named(crowded, number // 4), named(usual, number - number // 4 - 1))
    mixed = jax.random.permutation(jax.random.fold_in(own, 3), amount)
    giver, receiver = mixed[0:amount // 2 * 2:2], mixed[1:amount // 2 * 2:2]
    slack = jnp.minimum(sizes[giver] - 1, most - sizes[receiver]) // 2
    slack = jnp.where((giver == order[0]) | (receiver == order[0]) | (sizes[receiver] == 0), 0, jnp.maximum(slack, 0))
    passed = jax.random.randint(jax.random.fold_in(own, 4), (amount // 2,), 0, 1 << 20) % (slack + 1)
    sizes = sizes.at[giver].add(-passed).at[receiver].add(passed)
    members = jnp.searchsorted(jnp.cumsum(sizes), jnp.arange(rows * top), side="right").astype(jnp.int32)
    listing = members.reshape(top, rows).T
    listing = listing[jax.random.permutation(jax.random.fold_in(own, 1), rows)]
    rotation = jax.random.randint(jax.random.fold_in(own, 2), (rows, 1), 0, top)
    return jnp.take_along_axis(listing, (jnp.arange(top)[None, :] + rotation) % top, axis=1)


def load_shares(number_of, total, limit, slope, full):
    portions = [(1 << 20) // math.isqrt(rank ** slope) + 1 for rank in range(1, number_of + 1)]
    largest = limit if full else min(limit, max(-(-total // number_of), total * portions[0] // sum(portions)))
    least = 1 if total - largest >= number_of - 1 else 0
    given, spare = [largest] + [least] * (number_of - 1), total - largest - least * (number_of - 1)
    while spare > 0:
        free = [i for i in range(1, number_of) if given[i] < largest] or [i for i in range(1, number_of) if given[i] < limit]
        mass, budget = sum([portions[i] for i in free]), spare
        for i in free:
            more = min(limit - given[i], max(1, budget * portions[i] // mass), spare)
            given[i] = given[i] + more
            spare = spare - more
    return np.array(given)


def gaussian(stream_key, dims, width, bound, cuts=(), kind=jnp.bfloat16):
    values = width * jax.random.normal(stream_key, dims, jnp.float32)
    if cuts:
        values = values * block_levels(stream_key, dims, cuts, -0.22, 0.18)
    return jnp.clip(values, -bound, bound).astype(kind)


def setup_inputs(seed: int = 0) -> dict:
    streams_of = jax.random.split(jax.random.key(seed), 14)
    query_in = gaussian(streams_of[0], (WIDTH, SEQUENCE_LENGTH), 1.0, 6.0, ((0, 4), (1, 8)))
    key_in = draw_key_in(jax.random.fold_in(streams_of[13], 71), 0)
    value_in = gaussian(streams_of[2], (WIDTH, SEQUENCE_LENGTH), 1.0, 6.0, ((0, 4), (1, 8)))
    erase_pre = draw_erase_pre(jax.random.fold_in(streams_of[13], 71), 0)
    decay_pre = draw_decay_pre(jax.random.fold_in(streams_of[13], 71), 0)
    mix_gain = jnp.clip(1.0 + 0.18 * jax.random.normal(streams_of[5], (WIDTH,), jnp.float32), 0.1, 1.9)
    expert_in = gaussian(streams_of[6], (TOKENS, D), 1.0, 6.0, ((0, 8),))
    expert_gain = jnp.clip(1.0 + 0.18 * jax.random.normal(streams_of[7], (D,), jnp.float32), 0.1, 1.9)
    routes_keys = jax.random.split(jax.random.fold_in(streams_of[8], 1), TOKENS // TOK_EP)
    routes_turns = jax.random.permutation(jax.random.fold_in(streams_of[8], 3), TOKENS // TOK_EP)
    routes = jax.vmap(lambda own, number: shared_out(jax.random.fold_in(streams_of[8], 2), own, number, TOK_EP, EXPERTS, TOPK, CAP, 2))(routes_keys, routes_turns).reshape((TOKENS, TOPK))
    route_weight = jnp.clip(0.1 + 0.9 * jax.random.uniform(streams_of[9], (TOKENS, TOPK), jnp.float32) ** block_levels(streams_of[9], (TOKENS, TOPK), ((0, 8),), -0.2, 0.2), 0.1, 1.0)
    gate_weight = gaussian(streams_of[10], (EXPERTS, D, FFX), D ** -0.5, 0.125, ((0, 8), (2, 4)))
    up_weight = gaussian(streams_of[11], (EXPERTS, D, FFX), D ** -0.5, 0.125, ((0, 8), (2, 4)))
    down_weight = gaussian(streams_of[12], (EXPERTS, FFX, D), FFX ** -0.5, 0.09375, ((0, 8), (1, 4)))
    return {"query_in": query_in, "key_in": key_in, "value_in": value_in, "erase_pre": erase_pre, "decay_pre": decay_pre, "mix_gain": mix_gain, "expert_in": expert_in, "expert_gain": expert_gain, "routes": routes, "route_weight": route_weight, "gate_weight": gate_weight, "up_weight": up_weight, "down_weight": down_weight}


highest = lax.Precision.HIGHEST

def token_terms(key_in, erase_pre, decay_pre):
    key_f = key_in.astype(jnp.float32)
    unit_key = key_f * lax.rsqrt(lax.optimization_barrier(jnp.sum(key_f * key_f, axis=-1, keepdims=True)) + 1e-05)
    eraser = unit_key * jax.nn.sigmoid(erase_pre.astype(jnp.float32))
    log_keep = -jnp.exp(-jax.nn.softplus(-decay_pre.astype(jnp.float32)) - 0.5)
    return (key_f, unit_key, eraser, log_keep)

def advance(carried, inputs):
    query_f, key_f, value_f, unit_key, eraser, keep = inputs
    seen = jnp.einsum('hvk,hk->hv', carried, unit_key, precision=highest)
    carried = carried * keep[:, None, :] - seen[:, :, None] * eraser[:, None, :] + value_f[:, :, None] * key_f[:, None, :]
    return (carried, jnp.einsum('hvk,hk->hv', carried, query_f, precision=highest))

def mixer(query_in, key_in, value_in, erase_pre, decay_pre, mix_gain):
    layout = (SEQUENCE_LENGTH, HEADS, HEAD_DIM)
    query_f = query_in.astype(jnp.float32).reshape(layout)
    value_f = value_in.astype(jnp.float32).reshape(layout)
    key_f, unit_key, eraser, log_keep = token_terms(key_in.reshape(layout), erase_pre.reshape(layout), decay_pre.reshape(layout))
    inputs = (query_f, key_f, value_f, unit_key, eraser, jnp.exp(log_keep))
    initial = jnp.zeros((HEADS, HEAD_DIM, HEAD_DIM), jnp.float32)
    _, ahead = lax.scan(advance, initial, inputs)
    _, behind = lax.scan(advance, initial, inputs, reverse=True)
    summed = ahead + behind
    center = lax.optimization_barrier(jnp.mean(summed, axis=-1, keepdims=True))
    spread = lax.optimization_barrier(jnp.mean(jnp.square(summed - center), axis=-1, keepdims=True))
    scaled = (summed - center) * lax.rsqrt(spread + HEAD_DIM * 1e-05) * mix_gain.reshape(HEADS, HEAD_DIM)
    return scaled.astype(jnp.bfloat16).reshape(SEQUENCE_LENGTH, HEADS * HEAD_DIM)

def slot_targets(routes):
    onehot = (routes[:, :, None] == jnp.arange(EXPERTS, dtype=jnp.int32)[None, None, :]).astype(jnp.int32)
    flat = onehot.reshape(-1, EXPERTS)
    before = jnp.cumsum(flat, axis=0) - flat
    slot_index = lax.optimization_barrier(jnp.sum(before * flat, axis=-1)).reshape(routes.shape)
    return routes * CAP + slot_index

def dispatch_matrix(targets, slot_total):
    matches = targets[None, :, :] == jnp.arange(slot_total, dtype=jnp.int32)[:, None, None]
    return lax.optimization_barrier(jnp.sum(matches.astype(jnp.float32), axis=-1)).astype(jnp.bfloat16)

def experts_part(expert_in, expert_gain, routes, route_weight, gate_weight, up_weight, down_weight):
    input_f = expert_in.astype(jnp.float32)
    normed = (input_f * lax.rsqrt(lax.optimization_barrier(jnp.mean(input_f * input_f, axis=-1, keepdims=True)) + 1e-06) * expert_gain).astype(jnp.bfloat16)
    targets = jax.vmap(slot_targets)(routes.reshape(N_EP, TOK_EP, TOPK))

    def fill(pack):
        selected_experts, rows = pack
        return jnp.dot(dispatch_matrix(selected_experts, EXPERTS * CAP), rows, preferred_element_type=jnp.float32).astype(jnp.bfloat16)
    buffers = lax.map(fill, (targets, normed.reshape(N_EP, TOK_EP, D)))
    buffers = buffers.reshape(N_EP, EXPERTS, CAP, D).transpose(1, 0, 2, 3).reshape(EXPERTS, N_EP * CAP, D)

    def expert(pack):
        rows, gate_mat, up_mat, down_mat = pack
        gate_sum = jnp.dot(rows, gate_mat, preferred_element_type=jnp.float32)
        up_sum = jnp.dot(rows, up_mat, preferred_element_type=jnp.float32)
        hidden = (jax.nn.silu(gate_sum) * up_sum).astype(jnp.bfloat16)
        groups = hidden.reshape(-1, N_TP, FFX // N_TP).astype(jnp.float32)
        downs = down_mat.reshape(N_TP, FFX // N_TP, D).astype(jnp.float32)
        partial_value = jnp.einsum('rjf,jfd->jrd', groups, downs).astype(jnp.bfloat16)
        partial_value = lax.optimization_barrier(partial_value)
        return lax.optimization_barrier(jnp.sum(partial_value.astype(jnp.float32), axis=0)).astype(jnp.bfloat16)
    results = lax.map(expert, (buffers, gate_weight, up_weight, down_weight)).reshape(EXPERTS, N_EP, CAP, D)
    source = (jnp.arange(TOKENS, dtype=jnp.int32) // TOK_EP)[:, None]
    slot_index = targets.reshape(TOKENS, TOPK) - routes * CAP
    picked = results[routes, source, slot_index].astype(jnp.float32)
    return lax.optimization_barrier(jnp.sum(picked * route_weight[:, :, None], axis=1)).astype(jnp.bfloat16)

def reference(query_in, key_in, value_in, erase_pre, decay_pre, mix_gain, expert_in, expert_gain, routes, route_weight, gate_weight, up_weight, down_weight):
    mixer_out = mixer(query_in.T, key_in.T, value_in.T, erase_pre.T, decay_pre.T, mix_gain).T
    expert_out = experts_part(expert_in, expert_gain, routes, route_weight, gate_weight, up_weight, down_weight)
    return (mixer_out, expert_out)
```

```python
import math

import jax
import jax.numpy as jnp
from jax import lax
from jax.experimental import pallas as pl
from jax.experimental.pallas import tpu as pltpu
from jax.sharding import PartitionSpec as P

HEAD_DIM = 64


highest = lax.Precision.HIGHEST
SPAN = 128


def dot(left, right, dims=((1,), (0,)), precision=None):
    return lax.dot_general(
        left, right, (dims, ((), ())), precision=precision, preferred_element_type=jnp.float32
    )


def low(array):
    return array.astype(jnp.bfloat16)


TN = ((0,), (0,))
NT = ((1,), (1,))


def local_kernel(q_ref, k_ref, v_ref, e_ref, d_ref, read_ref, out_ref, step_ref, map_ref):
    channels, span = q_ref.shape
    heads = channels // HEAD_DIM
    row = lax.broadcasted_iota(jnp.int32, (span, span), 0)
    col = lax.broadcasted_iota(jnp.int32, (span, span), 1)
    crossed = row ^ col

    query_f = q_ref[...].astype(jnp.float32)
    key_f = k_ref[...].astype(jnp.float32)
    value = v_ref[...]
    log_keep = -math.exp(-0.5) / (1.0 + jnp.exp(-d_ref[...].astype(jnp.float32)))
    squares = (key_f * key_f).reshape(heads, HEAD_DIM, span)
    norm = lax.rsqrt(jnp.sum(squares, axis=1, keepdims=True) + 1e-05)
    unit = (key_f.reshape(heads, HEAD_DIM, span) * norm).reshape(channels, span)
    eraser = unit / (1.0 + jnp.exp(-e_ref[...].astype(jnp.float32)))

    upper = jnp.where(row <= col, 1.0, 0.0)
    cumulative = dot(log_keep, upper, precision=highest)
    prior = cumulative - log_keep
    total = cumulative[:, span - 1 :]
    middle = cumulative[:, span // 2 - 1 : span // 2]
    prior_up = jnp.exp(prior - middle)
    cum_down = jnp.exp(middle - cumulative)
    cum_up = jnp.exp(cumulative - middle)
    prior_down = jnp.exp(middle - prior)
    to_middle = jnp.exp(middle)
    from_middle = jnp.exp(total - middle)
    decay = jnp.exp(total)

    sides = (
        (unit * prior_up, query_f * cum_up, key_f * cum_down, eraser * cum_down,
         to_middle, from_middle, row < col, row <= col),
        (unit * cum_down, query_f * prior_down, key_f * prior_up, eraser * prior_up,
         from_middle, to_middle, row > col, row >= col),
    )
    units = []
    for side, (u, q, k, e, scale_in, scale_out, strict, inclusive) in enumerate(sides):
        u0, q0 = u * scale_in, q * scale_in
        for h in range(heads):
            at = slice(h * HEAD_DIM, (h + 1) * HEAD_DIM)
            uq = jnp.concatenate([low(u[at]), low(q[at])], axis=1)
            kb, eb = low(k[at]), low(e[at])
            mk = dot(kb, uq, TN)
            me = dot(eb, uq, TN)
            erase_mix = jnp.where(strict, me[:, :span], 0.0)
            units.append(
                dict(
                    side=side, h=h, at=at, kb=kb, eb=eb, u0=u0[at], q0=q0[at],
                    key_mix=low(jnp.where(strict, mk[:, :span], 0.0)),
                    key_read=low(jnp.where(inclusive, mk[:, span:], 0.0)),
                    erase_read=low(jnp.where(inclusive, me[:, span:], 0.0)),
                    erase_mix=erase_mix,
                    scale_out=scale_out[at], decay=decay[at],
                )
            )
    eye = jnp.where(row == col, 1.0, 0.0)
    solved = [eye - jnp.where(crossed == 1, m["erase_mix"], 0.0) for m in units]
    level = 1
    while (1 << level) < span:
        mask = (crossed >> level) == 1
        held = [low(x) for x in solved]
        half = [
            low(dot(x, low(jnp.where(mask, m["erase_mix"], 0.0)))) for x, m in zip(held, units)
        ]
        solved = [s - dot(y, x) for s, y, x in zip(solved, half, held)]
        level += 1

    outs = [None] * heads
    eye_k = jnp.where(
        lax.broadcasted_iota(jnp.int32, (HEAD_DIM, HEAD_DIM), 0)
        == lax.broadcasted_iota(jnp.int32, (HEAD_DIM, HEAD_DIM), 1),
        1.0,
        0.0,
    )
    for m, x in zip(units, solved):
        v = value[m["at"]]
        vm = dot(v, jnp.concatenate([m["key_mix"], m["key_read"]], axis=1))
        stacked = jnp.concatenate([low(vm[:, :span]), low(m["u0"])], axis=0)
        removed = low(dot(stacked, low(x)))
        taken = dot(removed, m["erase_read"])
        local = vm[:, span:] - taken[:HEAD_DIM]
        h, side = m["h"], m["side"]
        outs[h] = local if outs[h] is None else outs[h] + local
        read_ref[side, m["at"], :] = low(m["q0"] - taken[HEAD_DIM:])
        gone = dot(m["eb"], removed, NT)
        added = dot(m["kb"], v, NT)
        state = (added - gone[:, :HEAD_DIM]) * m["scale_out"]
        moved = eye_k * m["decay"] - gone[:, HEAD_DIM:] * m["scale_out"]
        step_ref[0, side, h] = jnp.concatenate([state, moved], axis=1)
    for h in range(heads):
        out_ref[h * HEAD_DIM : (h + 1) * HEAD_DIM, :] = outs[h]

    first = pl.program_id(0) == 0

    @pl.when(first)
    def _():
        map_ref[...] = step_ref[0]

    @pl.when(jnp.logical_not(first))
    def _():
        for h in range(heads):
            step = step_ref[0, 0, h]
            new = dot(step[:, HEAD_DIM:], map_ref[0, h], precision=highest)
            map_ref[0, h] = new + jnp.concatenate(
                [step[:, :HEAD_DIM], jnp.zeros_like(eye_k)], axis=1
            )
            before = map_ref[1, h]
            new = dot(before[:, HEAD_DIM:], step_ref[0, 1, h], precision=highest)
            map_ref[1, h] = new + jnp.concatenate(
                [before[:, :HEAD_DIM], jnp.zeros_like(eye_k)], axis=1
            )


def finish_kernel(maps_ref, step_ref, read_ref, local_ref, gain_ref, out_ref, enter_ref, states_ref):
    count = maps_ref.shape[0]
    heads = maps_ref.shape[2]
    blocks = step_ref.shape[0]
    mine = lax.axis_index("ep")
    enter_ref[...] = jnp.zeros_like(enter_ref)

    def gather(j, carry):
        for side, at in ((0, j), (1, count - 1 - j)):
            reached = at < mine if side == 0 else at > mine

            @pl.when(reached)
            def _():
                for h in range(heads):
                    part = maps_ref[at, side, h]
                    state = enter_ref[side, h]
                    high = low(state)
                    rest = low(state - high.astype(jnp.float32))
                    both = jnp.concatenate([high, rest], axis=1)
                    new = dot(part[:, HEAD_DIM:], both)
                    enter_ref[side, h] = (
                        new[:, :HEAD_DIM] + new[:, HEAD_DIM:] + part[:, :HEAD_DIM].astype(jnp.float32)
                    )

        return carry

    lax.fori_loop(0, count, gather, 0)

    def chain(j, carry):
        for side, at in ((0, j), (1, blocks - 1 - j)):
            for h in range(heads):
                step = step_ref[at, side, h]
                state = enter_ref[side, h]
                states_ref[at, h, side * HEAD_DIM : (side + 1) * HEAD_DIM, :] = low(state)
                enter_ref[side, h] = step[:, :HEAD_DIM] + dot(
                    step[:, HEAD_DIM:], state, precision=highest
                )
        return carry

    lax.fori_loop(0, blocks, chain, 0)

    def write(j, carry):
        tokens = pl.ds(pl.multiple_of(j * SPAN, SPAN), SPAN)
        for h in range(heads):
            at = slice(h * HEAD_DIM, (h + 1) * HEAD_DIM)
            reads = jnp.concatenate([read_ref[0, at, tokens], read_ref[1, at, tokens]], axis=0)
            summed = local_ref[at, tokens] + dot(states_ref[j, h], reads, TN)
            center = jnp.mean(summed, axis=0, keepdims=True)
            moved = summed - center
            spread = jnp.mean(moved * moved, axis=0, keepdims=True)
            scaled = moved * lax.rsqrt(spread + HEAD_DIM * 1e-05) * gain_ref[at, :]
            out_ref[at, tokens] = low(scaled)
        return carry

    lax.fori_loop(0, blocks, write, 0)


def mixer_half(query_in, key_in, value_in, erase_pre, decay_pre, mix_gain):
    channels, seq_len = query_in.shape
    heads = channels // HEAD_DIM
    blocks = seq_len // SPAN
    taken = pl.BlockSpec((channels, SPAN), lambda c: (0, c))
    f32 = jnp.float32
    reads, local, steps, maps = pl.pallas_call(
        local_kernel,
        grid=(blocks,),
        in_specs=[taken] * 5,
        out_specs=[
            pl.BlockSpec((2, channels, SPAN), lambda c: (0, 0, c)),
            taken,
            pl.BlockSpec((1, 2, heads, HEAD_DIM, 2 * HEAD_DIM), lambda c: (c, 0, 0, 0, 0)),
            pl.BlockSpec((2, heads, HEAD_DIM, 2 * HEAD_DIM), lambda c: (0, 0, 0, 0)),
        ],
        out_shape=[
            jax.ShapeDtypeStruct((2, channels, seq_len), jnp.bfloat16),
            jax.ShapeDtypeStruct((channels, seq_len), f32),
            jax.ShapeDtypeStruct((blocks, 2, heads, HEAD_DIM, 2 * HEAD_DIM), f32),
            jax.ShapeDtypeStruct((2, heads, HEAD_DIM, 2 * HEAD_DIM), f32),
        ],
        compiler_params=pltpu.CompilerParams(dimension_semantics=("arbitrary",)),
        cost_estimate=pl.CostEstimate(
            flops=int(4e10 * heads * blocks / 32), bytes_accessed=1 << 23, transcendentals=1 << 20
        ),
        name="mixer_local",
    )(query_in, key_in, value_in, erase_pre, decay_pre)
    gathered = lax.all_gather(maps.astype(jnp.bfloat16), "ep")
    return pl.pallas_call(
        finish_kernel,
        out_shape=jax.ShapeDtypeStruct((channels, seq_len), jnp.bfloat16),
        scratch_shapes=[
            pltpu.VMEM((2, heads, HEAD_DIM, HEAD_DIM), f32),
            pltpu.VMEM((blocks, heads, 2 * HEAD_DIM, HEAD_DIM), jnp.bfloat16),
        ],
        cost_estimate=pl.CostEstimate(
            flops=int(1e10 * heads * blocks / 32), bytes_accessed=1 << 23, transcendentals=1 << 14
        ),
        name="mixer_finish",
    )(gathered, steps, reads, local, mix_gain.reshape(channels, 1))


def slot_targets(routes, experts_n, capacity):
    onehot = (routes[:, :, None] == jnp.arange(experts_n, dtype=jnp.int32)[None, None, :]).astype(
        jnp.int32
    )
    flat = onehot.reshape(-1, experts_n)
    before = jnp.cumsum(flat, axis=0) - flat
    slot_index = jnp.sum(before * flat, axis=-1).reshape(routes.shape)
    return routes * capacity + slot_index


def dispatch_matrix(targets, slot_total):
    matches = targets[None, :, :] == jnp.arange(slot_total, dtype=jnp.int32)[:, None, None]
    return jnp.sum(matches.astype(jnp.float32), axis=-1).astype(jnp.bfloat16)


def expert_half(expert_in, expert_gain, routes, route_weight, gate_weight, up_weight, down_weight):
    experts_n = lax.axis_size("ep")
    row_count = expert_in.shape[0]
    capacity = 3 * routes.shape[1] * row_count // (2 * experts_n)
    slot_total = experts_n * capacity
    input_f = expert_in.astype(jnp.float32)
    normed = (
        input_f
        * lax.rsqrt(jnp.mean(input_f * input_f, axis=-1, keepdims=True) + 1e-06)
        * expert_gain
    ).astype(jnp.bfloat16)
    targets = slot_targets(routes, experts_n, capacity)
    buffer = jnp.dot(
        dispatch_matrix(targets, slot_total), normed, preferred_element_type=jnp.float32
    ).astype(jnp.bfloat16)
    gate_local = gate_weight[0]
    up_local = up_weight[0]
    down_local = down_weight[0]
    col_count = normed.shape[1] // lax.axis_size("tp")
    arrived = lax.all_to_all(
        buffer.reshape(experts_n, capacity, normed.shape[1]),
        "ep",
        split_axis=0,
        concat_axis=0,
        tiled=True,
    ).reshape(slot_total, normed.shape[1])
    gate_sum = jnp.dot(arrived, gate_local, preferred_element_type=jnp.float32)
    up_sum = jnp.dot(arrived, up_local, preferred_element_type=jnp.float32)
    hidden = (jax.nn.silu(gate_sum) * up_sum).astype(jnp.bfloat16)
    summed = lax.psum_scatter(
        lax.dot_general(
            down_local, hidden, (((0,), (1,)), ((), ())), preferred_element_type=jnp.float32
        ).astype(jnp.bfloat16),
        "tp",
        scatter_dimension=0,
        tiled=True,
    )
    returned = lax.all_to_all(
        summed.reshape(col_count, experts_n, capacity),
        "ep",
        split_axis=1,
        concat_axis=1,
        tiled=True,
    ).reshape(col_count, slot_total)
    matches = targets[:, :, None] == jnp.arange(slot_total, dtype=jnp.int32)[None, None, :]
    combine = jnp.sum(matches.astype(jnp.float32) * route_weight[:, :, None], axis=1)
    return jnp.einsum("tx,cx->tc", combine, returned.astype(jnp.float32), precision=highest).astype(
        jnp.bfloat16
    )


def on_device(
    query_in,
    key_in,
    value_in,
    erase_pre,
    decay_pre,
    mix_gain,
    expert_in,
    expert_gain,
    routes,
    route_weight,
    gate_weight,
    up_weight,
    down_weight,
):
    mixer_out = mixer_half(query_in, key_in, value_in, erase_pre, decay_pre, mix_gain)
    expert_out = expert_half(
        expert_in, expert_gain, routes, route_weight, gate_weight, up_weight, down_weight
    )
    return (mixer_out, expert_out)


def solution(mesh):
    placed = (
        P("tp", "ep"),
        P("tp", "ep"),
        P("tp", "ep"),
        P("tp", "ep"),
        P("tp", "ep"),
        P("tp"),
        P("ep", None),
        P(),
        P("ep", None),
        P("ep", None),
        P("ep", None, "tp"),
        P("ep", None, "tp"),
        P("ep", "tp", None),
    )
    return jax.shard_map(
        on_device,
        mesh=mesh,
        in_specs=placed,
        out_specs=(P("tp", "ep"), P("ep", "tp")),
        check_vma=False,
    )
```

```python
import math

import jax
import jax.numpy as jnp
from jax import lax
from jax.experimental import pallas as pl
from jax.experimental.pallas import tpu as pltpu
from jax.sharding import PartitionSpec as P

HEAD_DIM = 64


highest = lax.Precision.HIGHEST
SPAN = 128


def dot(left, right, dims=((1,), (0,)), precision=None):
    return lax.dot_general(
        left, right, (dims, ((), ())), precision=precision, preferred_element_type=jnp.float32
    )


def low(array):
    return array.astype(jnp.bfloat16)


TN = ((0,), (0,))
NT = ((1,), (1,))


def local_kernel(q_ref, k_ref, v_ref, e_ref, d_ref, read_ref, out_ref, step_ref, map_ref):
    channels, span = q_ref.shape
    heads = channels // HEAD_DIM
    row = lax.broadcasted_iota(jnp.int32, (span, span), 0)
    col = lax.broadcasted_iota(jnp.int32, (span, span), 1)
    crossed = row ^ col

    query_f = q_ref[...].astype(jnp.float32)
    key_f = k_ref[...].astype(jnp.float32)
    value = v_ref[...]
    log_keep = -math.exp(-0.5) / (1.0 + jnp.exp(-d_ref[...].astype(jnp.float32)))
    squares = (key_f * key_f).reshape(heads, HEAD_DIM, span)
    norm = lax.rsqrt(jnp.sum(squares, axis=1, keepdims=True) + 1e-05)
    unit = (key_f.reshape(heads, HEAD_DIM, span) * norm).reshape(channels, span)
    eraser = unit / (1.0 + jnp.exp(-e_ref[...].astype(jnp.float32)))

    upper = jnp.where(row <= col, 1.0, 0.0)
    cumulative = dot(log_keep, upper, precision=highest)
    prior = cumulative - log_keep
    total = cumulative[:, span - 1 :]
    middle = cumulative[:, span // 2 - 1 : span // 2]
    prior_up = jnp.exp(prior - middle)
    cum_down = jnp.exp(middle - cumulative)
    cum_up = jnp.exp(cumulative - middle)
    prior_down = jnp.exp(middle - prior)
    to_middle = jnp.exp(middle)
    from_middle = jnp.exp(total - middle)
    decay = jnp.exp(total)

    sides = (
        (unit * prior_up, query_f * cum_up, key_f * cum_down, eraser * cum_down,
         to_middle, from_middle, row < col, row <= col),
        (unit * cum_down, query_f * prior_down, key_f * prior_up, eraser * prior_up,
         from_middle, to_middle, row > col, row >= col),
    )
    units = []
    for side, (u, q, k, e, scale_in, scale_out, strict, inclusive) in enumerate(sides):
        u0, q0 = u * scale_in, q * scale_in
        for h in range(heads):
            at = slice(h * HEAD_DIM, (h + 1) * HEAD_DIM)
            uq = jnp.concatenate([low(u[at]), low(q[at])], axis=1)
            kb, eb = low(k[at]), low(e[at])
            mk = dot(kb, uq, TN)
            me = dot(eb, uq, TN)
            erase_mix = jnp.where(strict, me[:, :span], 0.0)
            units.append(
                dict(
                    side=side, h=h, at=at, kb=kb, eb=eb, u0=u0[at], q0=q0[at],
                    key_mix=low(jnp.where(strict, mk[:, :span], 0.0)),
                    key_read=low(jnp.where(inclusive, mk[:, span:], 0.0)),
                    erase_read=low(jnp.where(inclusive, me[:, span:], 0.0)),
                    erase_mix=erase_mix,
                    scale_out=scale_out[at], decay=decay[at],
                )
            )
    eye = jnp.where(row == col, 1.0, 0.0)
    solved = [eye - jnp.where(crossed == 1, m["erase_mix"], 0.0) for m in units]
    level = 1
    while (1 << level) < span:
        mask = (crossed >> level) == 1
        held = [low(x) for x in solved]
        half = [
            low(dot(x, low(jnp.where(mask, m["erase_mix"], 0.0)))) for x, m in zip(held, units)
        ]
        solved = [s - dot(y, x) for s, y, x in zip(solved, half, held)]
        level += 1

    outs = [None] * heads
    eye_k = jnp.where(
        lax.broadcasted_iota(jnp.int32, (HEAD_DIM, HEAD_DIM), 0)
        == lax.broadcasted_iota(jnp.int32, (HEAD_DIM, HEAD_DIM), 1),
        1.0,
        0.0,
    )
    for m, x in zip(units, solved):
        v = value[m["at"]]
        vm = dot(v, jnp.concatenate([m["key_mix"], m["key_read"]], axis=1))
        stacked = jnp.concatenate([low(vm[:, :span]), low(m["u0"])], axis=0)
        removed = low(dot(stacked, low(x)))
        taken = dot(removed, m["erase_read"])
        local = vm[:, span:] - taken[:HEAD_DIM]
        h, side = m["h"], m["side"]
        outs[h] = local if outs[h] is None else outs[h] + local
        read_ref[side, m["at"], :] = low(m["q0"] - taken[HEAD_DIM:])
        gone = dot(m["eb"], removed, NT)
        added = dot(m["kb"], v, NT)
        state = (added - gone[:, :HEAD_DIM]) * m["scale_out"]
        moved = eye_k * m["decay"] - gone[:, HEAD_DIM:] * m["scale_out"]
        step_ref[0, side, h] = jnp.concatenate([state, moved], axis=1)
    for h in range(heads):
        out_ref[h * HEAD_DIM : (h + 1) * HEAD_DIM, :] = outs[h]

    first = pl.program_id(0) == 0

    @pl.when(first)
    def _():
        map_ref[...] = step_ref[0]

    @pl.when(jnp.logical_not(first))
    def _():
        for h in range(heads):
            step = step_ref[0, 0, h]
            new = dot(step[:, HEAD_DIM:], map_ref[0, h], precision=highest)
            map_ref[0, h] = new + jnp.concatenate(
                [step[:, :HEAD_DIM], jnp.zeros_like(eye_k)], axis=1
            )
            before = map_ref[1, h]
            new = dot(before[:, HEAD_DIM:], step_ref[0, 1, h], precision=highest)
            map_ref[1, h] = new + jnp.concatenate(
                [before[:, :HEAD_DIM], jnp.zeros_like(eye_k)], axis=1
            )


def finish_kernel(maps_ref, step_ref, read_ref, local_ref, gain_ref, out_ref, enter_ref, states_ref):
    count = maps_ref.shape[0]
    heads = maps_ref.shape[2]
    blocks = step_ref.shape[0]
    mine = lax.axis_index("ep")
    enter_ref[...] = jnp.zeros_like(enter_ref)

    def gather(j, carry):
        for side, at in ((0, j), (1, count - 1 - j)):
            reached = at < mine if side == 0 else at > mine

            @pl.when(reached)
            def _():
                for h in range(heads):
                    part = maps_ref[at, side, h]
                    state = enter_ref[side, h]
                    high = low(state)
                    rest = low(state - high.astype(jnp.float32))
                    both = jnp.concatenate([high, rest], axis=1)
                    new = dot(part[:, HEAD_DIM:], both)
                    enter_ref[side, h] = (
                        new[:, :HEAD_DIM] + new[:, HEAD_DIM:] + part[:, :HEAD_DIM].astype(jnp.float32)
                    )

        return carry

    lax.fori_loop(0, count, gather, 0)

    def chain(j, carry):
        for side, at in ((0, j), (1, blocks - 1 - j)):
            for h in range(heads):
                step = step_ref[at, side, h]
                state = enter_ref[side, h]
                states_ref[at, h, side * HEAD_DIM : (side + 1) * HEAD_DIM, :] = low(state)
                enter_ref[side, h] = step[:, :HEAD_DIM] + dot(
                    step[:, HEAD_DIM:], state, precision=highest
                )
        return carry

    lax.fori_loop(0, blocks, chain, 0)

    def write(j, carry):
        tokens = pl.ds(pl.multiple_of(j * SPAN, SPAN), SPAN)
        for h in range(heads):
            at = slice(h * HEAD_DIM, (h + 1) * HEAD_DIM)
            reads = jnp.concatenate([read_ref[0, at, tokens], read_ref[1, at, tokens]], axis=0)
            summed = local_ref[at, tokens] + dot(states_ref[j, h], reads, TN)
            center = jnp.mean(summed, axis=0, keepdims=True)
            moved = summed - center
            spread = jnp.mean(moved * moved, axis=0, keepdims=True)
            scaled = moved * lax.rsqrt(spread + HEAD_DIM * 1e-05) * gain_ref[at, :]
            out_ref[at, tokens] = low(scaled)
        return carry

    lax.fori_loop(0, blocks, write, 0)


def mixer_local(query_in, key_in, value_in, erase_pre, decay_pre):
    channels, seq_len = query_in.shape
    heads = channels // HEAD_DIM
    blocks = seq_len // SPAN
    taken = pl.BlockSpec((channels, SPAN), lambda c: (0, c))
    f32 = jnp.float32
    reads, local, steps, maps = pl.pallas_call(
        local_kernel,
        grid=(blocks,),
        in_specs=[taken] * 5,
        out_specs=[
            pl.BlockSpec((2, channels, SPAN), lambda c: (0, 0, c)),
            taken,
            pl.BlockSpec((1, 2, heads, HEAD_DIM, 2 * HEAD_DIM), lambda c: (c, 0, 0, 0, 0)),
            pl.BlockSpec((2, heads, HEAD_DIM, 2 * HEAD_DIM), lambda c: (0, 0, 0, 0)),
        ],
        out_shape=[
            jax.ShapeDtypeStruct((2, channels, seq_len), jnp.bfloat16),
            jax.ShapeDtypeStruct((channels, seq_len), f32),
            jax.ShapeDtypeStruct((blocks, 2, heads, HEAD_DIM, 2 * HEAD_DIM), f32),
            jax.ShapeDtypeStruct((2, heads, HEAD_DIM, 2 * HEAD_DIM), f32),
        ],
        compiler_params=pltpu.CompilerParams(dimension_semantics=("arbitrary",)),
        cost_estimate=pl.CostEstimate(
            flops=int(4e10 * heads * blocks / 32), bytes_accessed=1 << 23, transcendentals=1 << 20
        ),
        name="mixer_local",
    )(query_in, key_in, value_in, erase_pre, decay_pre)
    return reads, local, steps, maps


def mixer_finish(gathered, steps, reads, local, mix_gain):
    channels, seq_len = local.shape
    blocks, _, heads = steps.shape[:3]
    f32 = jnp.float32
    return pl.pallas_call(
        finish_kernel,
        out_shape=jax.ShapeDtypeStruct((channels, seq_len), jnp.bfloat16),
        scratch_shapes=[
            pltpu.VMEM((2, heads, HEAD_DIM, HEAD_DIM), f32),
            pltpu.VMEM((blocks, heads, 2 * HEAD_DIM, HEAD_DIM), jnp.bfloat16),
        ],
        cost_estimate=pl.CostEstimate(
            flops=int(1e10 * heads * blocks / 32), bytes_accessed=1 << 23, transcendentals=1 << 14
        ),
        name="mixer_finish",
    )(gathered, steps, reads, local, mix_gain.reshape(channels, 1))


def slot_targets(routes, experts_n, capacity):
    onehot = (routes[:, :, None] == jnp.arange(experts_n, dtype=jnp.int32)[None, None, :]).astype(
        jnp.int32
    )
    flat = onehot.reshape(-1, experts_n)
    before = jnp.cumsum(flat, axis=0) - flat
    slot_index = jnp.sum(before * flat, axis=-1).reshape(routes.shape)
    return routes * capacity + slot_index


def dispatch_matrix(targets, slot_total):
    matches = targets[None, :, :] == jnp.arange(slot_total, dtype=jnp.int32)[:, None, None]
    return jnp.sum(matches.astype(jnp.float32), axis=-1).astype(jnp.bfloat16)


def expert_half(
    hold, expert_in, expert_gain, routes, route_weight, gate_weight, up_weight, down_weight
):
    experts_n = lax.axis_size("ep")
    row_count = expert_in.shape[0]
    capacity = 3 * routes.shape[1] * row_count // (2 * experts_n)
    slot_total = experts_n * capacity
    input_f = expert_in.astype(jnp.float32)
    normed = (
        input_f
        * lax.rsqrt(jnp.mean(input_f * input_f, axis=-1, keepdims=True) + 1e-06)
        * expert_gain
    ).astype(jnp.bfloat16)
    targets = slot_targets(routes, experts_n, capacity)
    col_count = normed.shape[1] // lax.axis_size("tp")
    mine = lax.dynamic_slice_in_dim(normed, lax.axis_index("tp") * col_count, col_count, 1)
    buffer = jnp.dot(
        dispatch_matrix(targets, slot_total), mine, preferred_element_type=jnp.float32
    ).astype(jnp.bfloat16)
    gate_local = gate_weight[0]
    up_local = up_weight[0]
    down_local = down_weight[0]
    share = lax.all_to_all(
        buffer.reshape(experts_n, capacity, col_count),
        "ep",
        split_axis=0,
        concat_axis=0,
        tiled=True,
    ).reshape(slot_total, col_count)
    arrived = lax.all_gather(share, "tp", axis=1, tiled=True)
    arrived, gathered = hold(arrived)
    gate_sum = jnp.dot(arrived, gate_local, preferred_element_type=jnp.float32)
    up_sum = jnp.dot(arrived, up_local, preferred_element_type=jnp.float32)
    hidden = (jax.nn.silu(gate_sum) * up_sum).astype(jnp.bfloat16)
    partial_sum = lax.dot_general(
        down_local, hidden, (((0,), (1,)), ((), ())), preferred_element_type=jnp.float32
    ).astype(jnp.bfloat16)
    partial_sum, gathered = lax.optimization_barrier((partial_sum, gathered))
    summed = lax.psum_scatter(
        partial_sum,
        "tp",
        scatter_dimension=0,
        tiled=True,
    )
    returned = lax.all_to_all(
        summed.reshape(col_count, experts_n, capacity),
        "ep",
        split_axis=1,
        concat_axis=1,
        tiled=True,
    ).reshape(col_count, slot_total)
    matches = targets[:, :, None] == jnp.arange(slot_total, dtype=jnp.int32)[None, None, :]
    combine = jnp.sum(matches.astype(jnp.float32) * route_weight[:, :, None], axis=1)
    result = jnp.einsum(
        "tx,cx->tc", combine, returned.astype(jnp.float32), precision=highest
    ).astype(jnp.bfloat16)
    return result, gathered


def on_device(
    query_in,
    key_in,
    value_in,
    erase_pre,
    decay_pre,
    mix_gain,
    expert_in,
    expert_gain,
    routes,
    route_weight,
    gate_weight,
    up_weight,
    down_weight,
):
    reads, local, steps, maps = mixer_local(query_in, key_in, value_in, erase_pre, decay_pre)

    def hold(arrived):
        held, sent = lax.optimization_barrier((arrived, maps.astype(jnp.bfloat16)))
        return held, lax.all_gather(sent, "ep")

    expert_out, gathered = expert_half(
        hold, expert_in, expert_gain, routes, route_weight, gate_weight, up_weight, down_weight
    )
    mixer_out = mixer_finish(gathered, steps, reads, local, mix_gain)
    return (mixer_out, expert_out)


def solution(mesh):
    placed = (
        P("tp", "ep"),
        P("tp", "ep"),
        P("tp", "ep"),
        P("tp", "ep"),
        P("tp", "ep"),
        P("tp"),
        P("ep", None),
        P(),
        P("ep", None),
        P("ep", None),
        P("ep", None, "tp"),
        P("ep", None, "tp"),
        P("ep", "tp", None),
    )
    return jax.shard_map(
        on_device,
        mesh=mesh,
        in_specs=placed,
        out_specs=(P("tp", "ep"), P("ep", "tp")),
        check_vma=False,
    )
```
